32 devices in a mesh: rep: 2 (over x), fs: 8 (over z, y), tp: 2 (over core).
Axes of the slice: x: 2, y: 2, z: 4, core: 2. Of those that a mesh axis runs over, the one named last changes fastest.
Arguments:
- inputs: bfloat16 [8192, 1024], P(('rep', 'fs', 'tp')), may hold values from -6 to 6
- up_proj: bfloat16 [1024, 4096], P('fs', 'tp'), may hold values from -0.1875 to 0.1875
- down_proj: bfloat16 [4096, 1024], P('tp', 'fs'), may hold values from -0.09375 to 0.09375
- out_cotangent: bfloat16 [8192, 1024], P(('rep', 'fs', 'tp')), may hold values from -6 to 6
Outputs:
- grad_inputs: bfloat16 [8192, 1024], P(('rep', 'fs', 'tp'))
- grad_up: float32 [1024, 4096], P('fs', 'tp')
- grad_down: float32 [4096, 1024], P('tp', 'fs')
- energy_up: float32 [1024], P('fs')
- energy_down: float32 [4096], P('tp')
The draws below stay inside these ranges and needn't reach their ends.
All inputs are finite; a program needn't handle non-finite values.
Results may differ from the reference program's by a relative error of at most 0.001.
Values may be sent and summed in bfloat16 or wider, within the bound.
A program may use at most 128 MiB of HBM per device.

```python
import jax
import jax.numpy as jnp
from jax import lax

D = 1024
FF = 4096
TOKENS = 8192


def raised(entries, key, source, target, parts, factor):
    owner, partner = [(jnp.arange(entries.shape[position]) // (entries.shape[position] // parts)).reshape([-1 if axis == position else 1 for axis in range(entries.ndim)]) for position in (source, target)]
    chosen = jax.random.permutation(key, parts)[partner]
    strong = (owner == chosen) | (owner == (partner + parts // 2) % parts)
    return jnp.where(strong, factor * entries, entries)


def level_of(rng, extent, shards, smallest, top_value):
    factor_of = 1.0
    for dim, blocks in shards:
        heights = jax.random.uniform(jax.random.fold_in(jax.random.fold_in(rng, 6), dim), (blocks,), jnp.float32, smallest / len(shards), top_value / len(shards))
        factor_of = factor_of * jnp.repeat(jnp.exp(heights), extent[dim] // blocks).reshape((-1,) + (1,) * (len(extent) - 1 - dim))
    return factor_of


def gaussian(rng, dims, width, bound, cuts=(), dtype=jnp.bfloat16):
    array = width * jax.random.normal(rng, dims, jnp.float32)
    if cuts:
        array = array * level_of(rng, dims, cuts, -0.22, 0.18)
    return jnp.clip(array, -bound, bound).astype(dtype)


def heavy_noise(key, shape, deviation, reach, split, heavy, held_as=jnp.bfloat16):
    entries = deviation * jax.random.normal(key, shape, jnp.float32)
    if split:
        entries = entries * level_of(key, shape, split, -0.22, 0.18)
    return jnp.clip(raised(entries, jax.random.fold_in(key, 3), *heavy), -reach, reach).astype(held_as)


def setup_inputs(seed: int = 0) -> dict:
    streams_of = jax.random.split(jax.random.key(seed), 5)
    return {
        "inputs": gaussian(streams_of[0], (TOKENS, D), 1.0, 6.0, ((0, 32),)),
        "up_proj": gaussian(streams_of[1], (D, FF), D ** -0.5, 0.1875, ((0, 8), (1, 2))),
        "down_proj": gaussian(streams_of[2], (FF, D), FF ** -0.5, 0.09375, ((0, 2), (1, 8))),
        "out_cotangent": heavy_noise(streams_of[3], (TOKENS, D), 1.0, 6.0, ((0, 32),), (0, 1, 32, 2.75)),
    }


def contract(left, right, left_dim, right_dim):
    return lax.dot_general(left, right, (((left_dim,), (right_dim,)), ((), ())), preferred_element_type=jnp.float32)


def reference(inputs, up_proj, down_proj, out_cotangent):
    factor = float(TOKENS) ** -0.5
    pre = jnp.dot(inputs, up_proj, preferred_element_type=jnp.float32)
    active = jnp.square(jax.nn.relu(pre)).astype(jnp.bfloat16)
    back = contract(out_cotangent, down_proj, 1, 1)
    grad_pre = (2.0 * jax.nn.relu(pre) * back).astype(jnp.bfloat16)
    grad_inputs = contract(grad_pre, up_proj, 1, 1).astype(jnp.bfloat16)
    grad_up = contract(inputs, grad_pre, 0, 0) * factor
    grad_down = contract(active, out_cotangent, 0, 0) * factor
    energy_up = jnp.sum(grad_up * grad_up, axis=1) / FF
    energy_down = jnp.sum(grad_down * grad_down, axis=1) / D
    return grad_inputs, grad_up, grad_down, energy_up, energy_down
```

```python
import jax
import jax.numpy as jnp
from jax import lax
from jax.sharding import PartitionSpec as P


def contract(left, right, left_dim, right_dim):
    return lax.dot_general(
        left, right, (((left_dim,), (right_dim,)), ((), ())), preferred_element_type=jnp.float32
    )


def swap(array, axis):
    return lax.ppermute(array, axis, [(0, 1), (1, 0)])


def body(inputs, up_proj, down_proj, out_cotangent):
    width = up_proj.shape[0] * lax.axis_size("fs")
    hidden = up_proj.shape[1] * lax.axis_size("tp")
    rows = inputs.shape[0]
    factor = float(
        rows * lax.axis_size("rep") * lax.axis_size("fs") * lax.axis_size("tp")
    ) ** (-0.5)
    rep = lax.axis_index("rep")
    part = up_proj.shape[1] // lax.axis_size("rep")

    up_share = lax.dynamic_slice_in_dim(up_proj, rep * part, part, 1)
    down_share = lax.dynamic_slice_in_dim(down_proj, rep * part, part, 0).T
    whole_up = lax.all_gather(up_share, "fs", axis=0, tiled=True)
    whole_down = lax.all_gather(down_share, "fs", axis=0, tiled=True)

    in_pair = jnp.concatenate([inputs, swap(inputs, "rep")], axis=0)
    cot_pair = jnp.concatenate([out_cotangent, swap(out_cotangent, "rep")], axis=0)
    tokens = jnp.concatenate([in_pair, swap(in_pair, "tp")], axis=0)
    cotangent = jnp.concatenate([cot_pair, swap(cot_pair, "tp")], axis=0)

    pre = jnp.dot(tokens, whole_up, preferred_element_type=jnp.float32)
    active = jnp.square(jax.nn.relu(pre)).astype(jnp.bfloat16)
    down_part = contract(cotangent, active, 0, 0) * factor
    down_sum = lax.psum_scatter(down_part, "fs", scatter_dimension=0, tiled=True)

    back = jnp.dot(cotangent, whole_down, preferred_element_type=jnp.float32)
    grad_pre = (2.0 * jax.nn.relu(pre) * back).astype(jnp.bfloat16)
    up_part = contract(tokens, grad_pre, 0, 0) * factor
    up_sum = lax.psum_scatter(up_part, "fs", scatter_dimension=0, tiled=True)

    partial = contract(grad_pre, whole_up, 1, 1)
    pair = partial[: 2 * rows] + swap(partial[2 * rows :], "tp")
    grad_inputs = (pair[:rows] + swap(pair[rows:], "rep")).astype(jnp.bfloat16)

    def both(mine):
        other = swap(mine, "rep")
        first = rep == 0
        return jnp.concatenate(
            [jnp.where(first, mine, other), jnp.where(first, other, mine)], axis=1
        )

    down_flip = both(down_sum)
    grad_down = jnp.transpose(down_flip)
    energy_down = lax.psum(jnp.sum(down_flip * down_flip, axis=0), "fs") / width
    grad_up = both(up_sum)
    energy_up = lax.psum(jnp.sum(grad_up * grad_up, axis=1), "tp") / hidden
    return (grad_inputs, grad_up, grad_down, energy_up, energy_down)


def solution(mesh):
    return jax.shard_map(
        body,
        mesh=mesh,
        in_specs=(
            P(("rep", "fs", "tp"), None),
            P("fs", "tp"),
            P("tp", "fs"),
            P(("rep", "fs", "tp"), None),
        ),
        out_specs=(P(("rep", "fs", "tp"), None), P("fs", "tp"), P("tp", "fs"), P("fs"), P("tp")),
        check_vma=False,
    )
```
